32 devices in a mesh: ep: 8 (over z, x), tp: 4 (over y, core).
Axes of the slice: x: 2, y: 2, z: 4, core: 2. Of those that a mesh axis runs over, the one named last changes fastest.
Arguments:
- tokens: bfloat16 [256, 4096], P('ep'), may hold values from -6 to 6
- routes: int32 [256, 4], P('ep'), may hold values from 0 to 7, all different within a row; in each aligned block of 32 rows (0 to 31, 32 to 63, ...) at most 24 rows name the same one
- mix_weights: float32 [256, 4], P('ep'), may hold values from 0.2 to 1
- pre_gain: float32 [4096], replicated, may hold values from 0.1 to 1.9
- gate_weight: bfloat16 [8, 4096, 2048], P('ep', None, 'tp'), may hold values from -0.09375 to 0.09375
- up_weight: bfloat16 [8, 4096, 2048], P('ep', None, 'tp'), may hold values from -0.09375 to 0.09375
- down_weight: bfloat16 [8, 2048, 4096], P('ep', 'tp'), may hold values from -1 to 1
- post_gain: float32 [4096], P('tp'), may hold values from 0.1 to 1.9
Outputs:
- layer_out: bfloat16 [256, 4096], P('ep', 'tp')
The draws below stay inside these ranges and needn't reach their ends.
Inputs may be any that keep to these rules, and one draw needn't show every extreme that they name: `routes`: within a row the 4 experts differ; among the rows of one index of ep no expert is named more than 24 times.
All inputs are finite; a program needn't handle non-finite values.
Results may differ from the reference program's by a relative error of at most 0.019.
Values may be sent and summed in bfloat16 or wider, within the bound.
A program may use at most 64 MiB of HBM per device.

```python
import math
import jax
import jax.numpy as jnp
import numpy as np
from jax import lax

D = 4096
FF = 2048
TOP = 4
TOK_DEV = 32
EXPERTS = 8
CAP = 24
TOKENS = 256
N_EP = 8
N_TP = 4


def draw_down_weight(key, part):
    noise = jnp.clip(jax.random.normal(jax.random.fold_in(key, 11), (EXPERTS, FF, D), jnp.float32), -6.0, 6.0)
    noise = noise * FF ** (-0.5)
    position = jnp.arange(D, dtype=jnp.float32) / D
    rise = 3.0 ** position * jax.random.uniform(jax.random.fold_in(key, 12), (D,), jnp.float32, 0.6, 1.6)
    return jnp.clip(noise * rise, -1.0, 1.0).astype(jnp.bfloat16)


def steps_of(key, shape, split, smallest, high):
    loudness = 1.0
    for axis_at, parts in split:
        steps = jax.random.uniform(jax.random.fold_in(jax.random.fold_in(key, 6), axis_at), (parts,), jnp.float32, smallest / len(split), high / len(split))
        loudness = loudness * jnp.repeat(jnp.exp(steps), shape[axis_at] // parts).reshape((-1,) + (1,) * (len(shape) - 1 - axis_at))
    return loudness


def assign_block(rng, own, number, rows, amount, top, most, skew):
    order = jax.random.permutation(rng, amount)
    packed, ordinary = portions_of(amount, rows * top, most, skew, True), portions_of(amount, rows * top, most, skew, False)
    places = jnp.arange(amount)

    def named(lengths, offset_by):
        used = int((lengths > 0).sum())
        fixed = max(1, used // 4)
        shifted = fixed + (places - fixed + offset_by * (used - fixed)) % max(1, amount - fixed)
        return jnp.zeros((amount,), jnp.int32).at[order[jnp.where(places < fixed, places, shifted)]].set(jnp.asarray(lengths, jnp.int32))

    lengths = jnp.where(number % 4 == 0, named(packed, number // 4), named(ordinary, number - number // 4 - 1))
    mixed = jax.random.permutation(jax.random.fold_in(own, 3), amount)
    giver, taker = mixed[0:amount // 2 * 2:2], mixed[1:amount // 2 * 2:2]
    margin = jnp.minimum(lengths[giver] - 1, most - lengths[taker]) // 2
    margin = jnp.where((giver == order[0]) | (taker == order[0]) | (lengths[taker] == 0), 0, jnp.maximum(margin, 0))
    shifted = jax.random.randint(jax.random.fold_in(own, 4), (amount // 2,), 0, 1 << 20) % (margin + 1)
    lengths = lengths.at[giver].add(-shifted).at[taker].add(shifted)
    labels = jnp.searchsorted(jnp.cumsum(lengths), jnp.arange(rows * top), side="right").astype(jnp.int32)
    grid = labels.reshape(top, rows).T
    grid = grid[jax.random.permutation(jax.random.fold_in(own, 1), rows)]
    offset_by = jax.random.randint(jax.random.fold_in(own, 2), (rows, 1), 0, top)
    return jnp.take_along_axis(grid, (jnp.arange(top)[None, :] + offset_by) % top, axis=1)


def portions_of(amount, total, limit, lean, full):
    portions = [(1 << 20) // math.isqrt(rank ** lean) + 1 for rank in range(1, amount + 1)]
    largest = limit if full else min(limit, max(-(-total // amount), total * portions[0] // sum(portions)))
    least = 1 if total - largest >= amount - 1 else 0
    given, surplus = [largest] + [least] * (amount - 1), total - largest - least * (amount - 1)
    while surplus > 0:
        free = [i for i in range(1, amount) if given[i] < largest] or [i for i in range(1, amount) if given[i] < limit]
        mass, left = sum([portions[i] for i in free]), surplus
        for i in free:
            extra = min(limit - given[i], max(1, left * portions[i] // mass), surplus)
            given[i] = given[i] + extra
            surplus = surplus - extra
    return np.array(given)


def bell_draw(own_key, extent, deviation, most, split=(), kind=jnp.bfloat16):
    level = steps_of(own_key, extent, split, -0.22, 0.18) if split else 1.0
    values = jax.random.normal(own_key, extent, jnp.float32) * deviation * level
    return jnp.minimum(jnp.maximum(values, -most), most).astype(kind)


def setup_inputs(seed: int = 0) -> dict:
    streams_of = jax.random.split(jax.random.key(seed), 9)
    tokens = bell_draw(streams_of[0], (TOKENS, D), 1.0, 6.0, ((0, 8),))
    routes_keys = jax.random.split(jax.random.fold_in(streams_of[1], 1), TOKENS // TOK_DEV)
    routes_turns = jax.random.permutation(jax.random.fold_in(streams_of[1], 3), TOKENS // TOK_DEV)
    routes = jax.vmap(lambda own, number: assign_block(jax.random.fold_in(streams_of[1], 2), own, number, TOK_DEV, EXPERTS, TOP, CAP, 2))(routes_keys, routes_turns).reshape((TOKENS, TOP))
    mix_weights = jnp.clip(0.2 + 0.8 * jax.random.uniform(streams_of[2], (TOKENS, TOP), jnp.float32) ** steps_of(streams_of[2], (TOKENS, TOP), ((0, 8),), -0.2, 0.2), 0.2, 1.0)
    pre_gain = jnp.clip(1.0 + 0.18 * jax.random.normal(streams_of[3], (D,), jnp.float32), 0.1, 1.9)
    gate_weight = bell_draw(streams_of[4], (EXPERTS, D, FF), D ** -0.5, 0.09375, ((0, 8), (2, 4)))
    up_weight = bell_draw(streams_of[5], (EXPERTS, D, FF), D ** -0.5, 0.09375, ((0, 8), (2, 4)))
    down_weight = draw_down_weight(jax.random.fold_in(streams_of[8], 71), 0)
    post_gain = jnp.clip(1.0 + 0.18 * jax.random.normal(streams_of[7], (D,), jnp.float32), 0.1, 1.9)
    return dict(tokens=tokens, routes=routes, mix_weights=mix_weights, pre_gain=pre_gain, gate_weight=gate_weight, up_weight=up_weight, down_weight=down_weight, post_gain=post_gain)


epsilon = 1e-06

def reference(tokens, routes, mix_weights, pre_gain, gate_weight, up_weight, down_weight, post_gain):
    floats = tokens.astype(jnp.float32)
    normed = (floats * lax.rsqrt(lax.optimization_barrier(jnp.mean(floats * floats, axis=-1, keepdims=True)) + epsilon) * pre_gain).astype(jnp.bfloat16)
    row_slots = N_EP * CAP
    group_width = FF // N_TP

    def visit_expert(result, per_expert):
        w_gate, w_up, w_down, expert_id = per_expert
        matches = routes == expert_id
        weight = lax.optimization_barrier(jnp.sum(jnp.where(matches, mix_weights, 0.0), axis=1))
        is_named = jnp.any(matches, axis=1)
        row_index = jnp.nonzero(is_named, size=row_slots, fill_value=0)[0].astype(jnp.int32)
        is_live = jnp.arange(row_slots) < jnp.sum(is_named.astype(jnp.int32))
        picked = normed[row_index]
        gate_act = jnp.dot(picked, w_gate, preferred_element_type=jnp.float32)
        up_act = jnp.dot(picked, w_up, preferred_element_type=jnp.float32)
        hidden = (jax.nn.silu(gate_act) * up_act).astype(jnp.bfloat16)
        pieces = jnp.einsum('rgf,gfd->grd', hidden.reshape(row_slots, N_TP, group_width).astype(jnp.float32), w_down.reshape(N_TP, group_width, D).astype(jnp.float32))
        pieces = lax.optimization_barrier(pieces.astype(jnp.bfloat16)).astype(jnp.float32)
        expert_out = lax.optimization_barrier(lax.optimization_barrier(jnp.sum(pieces, axis=0)).astype(jnp.bfloat16)).astype(jnp.float32)
        weighting = jnp.where(is_live, weight[row_index], 0.0)
        result = result.at[row_index].add(weighting[:, None] * expert_out)
        return (result, None)
    start = jnp.zeros((tokens.shape[0], D), jnp.float32)
    mixed, _ = lax.scan(visit_expert, start, (gate_weight, up_weight, down_weight, jnp.arange(EXPERTS, dtype=jnp.int32)))
    scale = lax.rsqrt(lax.optimization_barrier(jnp.mean(mixed * mixed, axis=-1, keepdims=True)) + epsilon)
    return (mixed * scale * post_gain).astype(jnp.bfloat16)
```

```python
import functools

import jax
import jax.numpy as jnp
from jax import lax
from jax.experimental import pallas as pl
from jax.experimental.pallas import tpu as pltpu
from jax.sharding import PartitionSpec as P

epsilon = 1e-06
CORES = 2
MESH = pl.DeviceIdType.MESH
VMEM_BYTES = 60 * 1024 * 1024
SUB = 1
OUT = [('z', 1), ('x', 0), ('z', 2), ('z', 3), ('xb', 0), ('zb', 1)]
XB = []
EVENTS = [('x', 0, 0), ('z', 1, 0), ('z', 2, 0), ('z', 3, 0), ('x', 1, 0), ('x', 2, 0), ('x', 3, 0), ('v', 1, 0), ('v', 2, 0), ('w', 0, 0), ('v', 3, 0), ('w', 1, 0), ('w', 2, 0), ('w', 3, 0)]


def fused_kernel(
    S, X, NT,
    tokens_hbm, routes_hbm, mix_hbm, pre_hbm, gate_hbm, up_hbm, down_hbm, post_hbm, out,
    tok, rt, mx, pre, post, xg, wg, wu, wd, wp, acc_g, acc_u, hid, hidp, wt, wr, weight,
    part, ya, yar, xb, xbr, xa, xar, yb, ybr, keep_a, keep_b, za, zar, zb, zbr, st,
    insem, wsem, ssem, gsem, psem, mixsem, hidsem, yarsem, xbrsem, xarsem, ybrsem, zsem, stsem,
):
    R, Dq = tok.shape[1], tok.shape[2]
    D = Dq * NT
    Z = S // X
    H = Dq // 2
    K = rt.shape[0]
    R2 = R // SUB
    me, t = lax.axis_index("ep"), lax.axis_index("tp")
    z, x = me // X, lax.rem(me, X)
    y, c = t // CORES, lax.rem(t, CORES)
    f32, bf16 = jnp.float32, jnp.bfloat16

    def flip(v, m):
        for b in range(m.bit_length()):
            if m >> b & 1:
                v = v + (1 << b) * (1 - 2 * lax.rem(v // (1 << b), 2))
        return v

    zs, xs, ys = [flip(z, d) for d in range(Z)], [x, 1 - x], [y, 1 - y]
    cs = [c, 1 - c]
    quarters = [ys[0] * CORES + cs[0], ys[0] * CORES + cs[1], ys[1] * CORES + cs[0], ys[1] * CORES + cs[1]]

    def peer(d, dx):
        return (zs[d] * X + xs[dx], t)

    across, partner = (me, quarters[2]), (me, quarters[1])
    beside = peer(0, 1)

    barrier = pltpu.get_barrier_semaphore()
    everyone = [peer(d, dx) for d in range(Z) for dx in range(X) if d or dx] + [(me, q) for q in quarters[1:]]
    for device in everyone:
        pl.semaphore_signal(barrier, inc=1, device_id=device, device_id_type=MESH)

    def span(q):
        return pl.ds(pl.multiple_of(q * Dq, Dq), Dq)

    first = [pltpu.make_async_copy(tokens_hbm.at[:, span(q)], tok.at[k], insem.at[0]) for k, q in enumerate(quarters)]
    first += [pltpu.make_async_copy(pre_hbm.at[:, span(q)], pre.at[k], insem.at[1]) for k, q in enumerate(quarters)]
    second = [
        pltpu.make_async_copy(routes_hbm, rt, insem.at[2]),
        pltpu.make_async_copy(mix_hbm, mx, insem.at[3]),
        pltpu.make_async_copy(post_hbm, post, insem.at[4]),
    ]
    for copy in first + second:
        copy.start()
    pltpu.make_async_copy(tok, tok, insem.at[0]).wait()
    pltpu.make_async_copy(pre, pre, insem.at[1]).wait()
    for copy in second:
        copy.wait()
    for k, q in enumerate(quarters):
        pltpu.make_async_copy(gate_hbm.at[0, span(q)], wg.at[k], wsem.at[k]).start()
        pltpu.make_async_copy(up_hbm.at[0, span(q)], wu.at[k], wsem.at[k]).start()
    for k, q in enumerate((quarters[0], quarters[2])):
        pltpu.make_async_copy(down_hbm.at[0, :, span(q)], wd.at[k], wsem.at[NT + k]).start()

    squares = jnp.zeros((R, 1), f32)
    for k in range(NT):
        floats = tok[k].astype(f32)
        squares = squares + jnp.sum(floats * floats, axis=1, keepdims=True)
    inv = lax.rsqrt(squares / D + epsilon)
    for k in range(NT):
        xg[k, 0:R, :] = (tok[k].astype(f32) * inv * pre[k]).astype(bf16)

    chosen, mixing = rt[...], mx[...]
    for d in range(Z):
        for dx in range(X):
            e = zs[d] * X + xs[dx]
            dense = jnp.zeros((1, R), f32)
            for k in range(K):
                dense = dense + jnp.where(chosen[k : k + 1, :] == e, mixing[k : k + 1, :], 0.0)
            wt[d * X + dx] = jnp.concatenate([dense, jnp.zeros((1, 128 - R), f32)], axis=1)
    wr[0] = wt[0]

    sent = [0, 0, 0]

    def bytes_of(ref):
        n = 1
        for size in ref.shape:
            n *= size
        return n * jnp.dtype(ref.dtype).itemsize

    def send(group, src, dst, recv_sem, device):
        pltpu.make_async_remote_copy(
            src_ref=src, dst_ref=dst, send_sem=ssem.at[group], recv_sem=recv_sem,
            device_id=device, device_id_type=MESH,
        ).start()
        sent[group] += bytes_of(src)

    def arrived(ref, sem):
        pltpu.make_async_copy(ref, ref, sem).wait()

    def block(k, b, i):
        return xg.at[k, b * R + i * R2 : b * R + (i + 1) * R2]

    def slot(half, b, i):
        return gsem.at[(half * (S - 1) + b - 1) * SUB + i]

    pl.semaphore_wait(barrier, len(everyone))

    for i in range(SUB):
        for kind, d in OUT:
            if kind == "z":
                send(0, block(0, 0, i), block(0, d * X, i), slot(0, d * X, i), peer(d, 0))
            elif kind == "zb":
                send(0, block(2, 0, i), block(2, d * X, i), slot(1, d * X, i), peer(d, 0))
            elif kind == "x":
                send(0, block(0, 0, i), block(0, 1, i), slot(0, 1, i), beside)
            elif kind == "xb":
                send(0, block(2, 0, i), block(2, 1, i), slot(1, 1, i), beside)
    for k, q in enumerate((quarters[1], quarters[3])):
        send(1, down_hbm.at[0, :, span(q)], wp.at[k], wsem.at[NT + 2 + k], partner)
    for b in range(1, S):
        send(2, wt.at[b], wr.at[b], mixsem.at[0], peer(b // X, b % X))

    by_z = [d for kind, d in OUT if kind == "zb"]
    by_x = [0] * any(kind == "xb" for kind, d in OUT) + XB

    def handle(kind, d, i):
        dx = 1 if kind[0] in "xw" else 0
        half = 0 if kind in "zx" else 1
        b = d * X + dx
        arrived(block(2 * half, b, i), slot(half, b, i))
        if dx == 0 and (half == 0 or d in by_x):
            send(0, block(2 * half, b, i), block(2 * half, b + 1, i), slot(half, b + 1, i), beside)
        if half == 0 and d not in (by_x if dx else by_z):
            send(0, block(0, b, i), block(2, b, i), slot(1, b, i), across)
        send(0, block(2 * half, b, i), block(2 * half + 1, b, i), psem.at[half], partner)

    def run(events):
        for kind, d, i in events:
            handle(kind, d, i)

    def multiply(k, start):
        both = pltpu.make_async_copy(wg.at[0], wg.at[0], wsem.at[k])
        both.wait()
        both.wait()
        for w, acc in ((wg, acc_g), (wu, acc_u)):
            product = jnp.dot(xg[k], w[k], preferred_element_type=f32)
            acc[...] = product if start else acc[...] + product

    late = [e for e in EVENTS if not (e[0] in "zx")]
    cut = max(n for n, e in enumerate(EVENTS) if e[0] in "zx") + 1
    run(EVENTS[:cut])
    multiply(0, True)
    arrived(xg.at[1, R : S * R], psem.at[0])
    multiply(1, False)
    arrived(wr.at[1:S], mixsem.at[0])
    named = jnp.concatenate([wr[b] for b in range(S)] + [jnp.zeros((128 - S, 128), f32)], axis=0)
    columns = jnp.transpose(named)
    for b in range(S):
        weight[b * R : (b + 1) * R] = jnp.broadcast_to(columns[:R, b : b + 1], (R, 128))
    run(EVENTS[cut:])
    multiply(2, False)
    arrived(xg.at[3, R : S * R], psem.at[1])
    multiply(3, False)

    F = hid.shape[1]
    half_rows = S * R // 2
    for i in range(2):
        rows = slice(i * half_rows, (i + 1) * half_rows)
        for at in range(0, F, 128):
            cols = slice(at, at + 128)
            gate = acc_g[rows, cols]
            hid[rows, cols] = (gate / (1.0 + jnp.exp(-gate)) * acc_u[rows, cols] * weight[rows]).astype(bf16)
        send(1, hid.at[rows], hidp.at[rows], hidsem.at[i], partner)
    for k in (1, 0):
        arrived(wd.at[k], wsem.at[NT + k])
        part[k] = jnp.dot(hid[...], wd[k], preferred_element_type=f32)
    for k in (1, 0):
        arrived(wp.at[k], wsem.at[NT + 2 + k])
    for i in range(2):
        rows = slice(i * half_rows, (i + 1) * half_rows)
        arrived(hidp.at[rows], hidsem.at[i])
    order = [d for d in range(1, Z)] + [0]
    for k in (1, 0):
        part[k] = part[k] + jnp.dot(hidp[...], wp[k], preferred_element_type=f32)
        for d in order:
            for dx in range(X):
                b = d * X + dx
                rows = slice(b * R, (b + 1) * R)
                if k:
                    ya[b] = part[k, rows, :H].astype(bf16)
                    send(1, ya.at[b], yar.at[b], yarsem.at[d], across)
                if dx:
                    xb[k, d] = part[k, rows, H:].astype(bf16)
                    send(1, xb.at[k, d], xbr.at[k, d], xbrsem.at[d], beside)

    for d in order:
        arrived(yar.at[d * X : (d + 1) * X], yarsem.at[d])
        for dx in (1, 0):
            b = d * X + dx
            total = part[0, b * R : (b + 1) * R, :H] + yar[b].astype(f32)
            if dx:
                xa[d] = total.astype(bf16)
                send(1, xa.at[d], xar.at[d], xarsem.at[d], beside)
            else:
                keep_a[d] = total
        arrived(xbr.at[:, d], xbrsem.at[d])
        for k in (1, 0):
            rows = slice(d * X * R, (d * X + 1) * R)
            total = part[k, rows, H:] + xbr[k, d].astype(f32)
            if k:
                yb[d] = total.astype(bf16)
                send(1, yb.at[d], ybr.at[d], ybrsem.at[d], across)
            else:
                keep_b[d] = total
    for d in order:
        arrived(xar.at[d], xarsem.at[d])
        total = keep_a[d] + xar[d].astype(f32)
        if d:
            za[d] = total.astype(bf16)
            send(1, za.at[d], zar.at[d], zsem.at[2 * d - 2], peer(d, 0))
        else:
            mine_a = total
        arrived(ybr.at[d], ybrsem.at[d])
        total = keep_b[d] + ybr[d].astype(f32)
        if d:
            zb[d] = total.astype(bf16)
            send(1, zb.at[d], zbr.at[d], zsem.at[2 * d - 1], peer(d, 0))
        else:
            mine_b = total
    for d in range(1, Z):
        arrived(zar.at[d], zsem.at[2 * d - 2])
        mine_a = mine_a + zar[d].astype(f32)
        arrived(zbr.at[d], zsem.at[2 * d - 1])
        mine_b = mine_b + zbr[d].astype(f32)

    squares = jnp.sum(mine_a * mine_a, axis=1, keepdims=True) + jnp.sum(mine_b * mine_b, axis=1, keepdims=True)
    st[0] = jnp.broadcast_to(squares, (R, 128))
    for k in range(1, NT):
        send(1, st.at[0], st.at[k], stsem.at[0], (me, quarters[k]))
    arrived(st.at[1:NT], stsem.at[0])
    for k in range(1, NT):
        squares = squares + st[k][:, 0:1]
    scale = lax.rsqrt(squares / D + epsilon)
    out[:, :H] = (mine_a * scale * post[:, :H]).astype(bf16)
    out[:, H:] = (mine_b * scale * post[:, H:]).astype(bf16)
    for group in (0, 1):
        span_of = gate_hbm.at[0, 0 : sent[group] // (2 * F)]
        arrived(span_of, ssem.at[group])
    arrived(wt.at[1:S], ssem.at[2])


def fused(S, X, NT, tokens, routes, mix_weights, pre_gain, gate_weight, up_weight, down_weight, post_gain):
    R, D = tokens.shape
    K = routes.shape[1]
    F = gate_weight.shape[2]
    Dq = D // NT
    H = Dq // 2
    Z = S // X
    f32, bf16 = jnp.float32, jnp.bfloat16
    dma, vmem = pltpu.SemaphoreType.DMA, pltpu.VMEM
    in_hbm = pl.BlockSpec(memory_space=pltpu.HBM)
    return pl.pallas_call(
        functools.partial(fused_kernel, S, X, NT),
        out_shape=jax.ShapeDtypeStruct((R, Dq), bf16),
        in_specs=[in_hbm] * 8,
        out_specs=pl.BlockSpec(memory_space=pltpu.VMEM),
        scratch_shapes=[
            vmem((NT, R, Dq), bf16),
            vmem((K, R), jnp.int32),
            vmem((K, R), f32),
            vmem((NT, 1, Dq), f32),
            vmem((1, Dq), f32),
            vmem((NT, S * R, Dq), bf16),
            vmem((NT, Dq, F), bf16),
            vmem((NT, Dq, F), bf16),
            vmem((2, F, Dq), bf16),
            vmem((2, F, Dq), bf16),
            vmem((S * R, F), f32),
            vmem((S * R, F), f32),
            vmem((S * R, F), bf16),
            vmem((S * R, F), bf16),
            vmem((S, 1, 128), f32),
            vmem((S, 1, 128), f32),
            vmem((S * R, 128), f32),
            vmem((2, S * R, Dq), f32),
            vmem((S, R, H), bf16),
            vmem((S, R, H), bf16),
            vmem((2, Z, R, H), bf16),
            vmem((2, Z, R, H), bf16),
            vmem((Z, R, H), bf16),
            vmem((Z, R, H), bf16),
            vmem((Z, R, H), bf16),
            vmem((Z, R, H), bf16),
            vmem((Z, R, H), f32),
            vmem((Z, R, H), f32),
            vmem((Z, R, H), bf16),
            vmem((Z, R, H), bf16),
            vmem((Z, R, H), bf16),
            vmem((Z, R, H), bf16),
            vmem((NT, R, 128), f32),
            dma((5,)),
            dma((NT + 4,)),
            dma((3,)),
            dma((2 * (S - 1) * SUB,)),
            dma((2,)),
            dma((1,)),
            dma((2,)),
            dma((Z,)),
            dma((Z,)),
            dma((Z,)),
            dma((Z,)),
            dma((2 * (Z - 1),)),
            dma((1,)),
        ],
        compiler_params=pltpu.CompilerParams(
            collective_id=0, has_side_effects=True, vmem_limit_bytes=VMEM_BYTES
        ),
    )(
        tokens, routes.T, mix_weights.T, pre_gain.reshape(1, D), gate_weight, up_weight, down_weight,
        post_gain.reshape(1, Dq),
    )


def routed(
    tokens, routes, mix_weights, pre_gain, gate_weight, up_weight, down_weight, post_gain
):
    tok_rows, width = tokens.shape
    top_count = routes.shape[1]
    experts = lax.axis_size("ep")
    capacity = min(tok_rows, max(2, (3 * tok_rows * top_count + 2 * experts - 1) // (2 * experts)))
    floats = tokens.astype(jnp.float32)
    normed = (
        floats * lax.rsqrt(jnp.mean(floats * floats, axis=-1, keepdims=True) + epsilon) * pre_gain
    ).astype(jnp.bfloat16)
    chosen = routes.reshape(-1)
    onehot = (chosen[:, None] == jnp.arange(experts, dtype=jnp.int32)[None, :]).astype(jnp.int32)
    before = jnp.cumsum(onehot, axis=0) - onehot
    slot_rank = jnp.sum(before * onehot, axis=1)
    target = chosen * capacity + slot_rank
    placed = target[:, None] == jnp.arange(experts * capacity, dtype=jnp.int32)[None, :]
    by_choice = placed.reshape(tok_rows, top_count, experts * capacity)
    picked = jnp.any(by_choice, axis=1).astype(jnp.bfloat16)
    outgoing = jnp.einsum("tc,td->cd", picked, normed, preferred_element_type=jnp.float32).astype(
        jnp.bfloat16
    )
    outgoing = outgoing.reshape(experts, capacity, width)
    slice_width = width // lax.axis_size("tp")
    outgoing_part = lax.dynamic_slice_in_dim(
        outgoing, lax.axis_index("tp") * slice_width, slice_width, 2
    )
    arrived = lax.all_to_all(outgoing_part, "ep", split_axis=0, concat_axis=0, tiled=True)
    arrived = lax.all_gather(arrived, "tp", axis=2, tiled=True)
    arrived_rows = arrived.reshape(experts * capacity, width)
    gate_act = jnp.dot(arrived_rows, gate_weight[0], preferred_element_type=jnp.float32)
    up_act = jnp.dot(arrived_rows, up_weight[0], preferred_element_type=jnp.float32)
    hidden = (jax.nn.silu(gate_act) * up_act).astype(jnp.bfloat16)
    partial_value = jnp.dot(hidden, down_weight[0], preferred_element_type=jnp.float32)
    summed = lax.psum_scatter(
        partial_value.astype(jnp.bfloat16), "tp", scatter_dimension=1, tiled=True
    )
    returned = lax.all_to_all(
        summed.reshape(experts, capacity, summed.shape[1]),
        "ep",
        split_axis=0,
        concat_axis=0,
        tiled=True,
    )
    results = returned.reshape(experts * capacity, summed.shape[1]).astype(jnp.float32)
    mixing = jnp.sum(mix_weights[:, :, None] * by_choice.astype(jnp.float32), axis=1)
    mixed = jnp.dot(mixing, results, precision=lax.Precision.HIGHEST)
    squares = jnp.sum(mixed * mixed, axis=1)
    total = lax.psum(squares, "tp")
    scale = lax.rsqrt(total / width + epsilon)
    return (mixed * scale[:, None] * post_gain).astype(jnp.bfloat16)


def solution(mesh):
    in_specs = (
        P("ep", None),
        P("ep", None),
        P("ep", None),
        P(),
        P("ep", None, "tp"),
        P("ep", None, "tp"),
        P("ep", "tp", None),
        P("tp"),
    )
    out_specs = P("ep", "tp")
    S, NT = mesh.shape["ep"], mesh.shape["tp"]
    X = 2
    on_device = routed
    if (S, NT) == (4 * X, 2 * CORES):
        on_device = functools.partial(fused, S, X, NT)
    return jax.shard_map(
        on_device, mesh=mesh, in_specs=in_specs, out_specs=out_specs, check_vma=False
    )
```
